32 devices in a mesh: ra: 4 (over z), cb: 8 (over y, x, core).
Axes of the slice: x: 2, y: 2, z: 4, core: 2. Of those that a mesh axis runs over, the one named last changes fastest.
Arguments:
- tokens: bfloat16 [512, 3072], P(None, 'ra'), may hold values from -14 to 14, as said below
- norm_gain: float32 [2, 3072], P(None, 'ra'), may hold values from 0.1 to 1.9
- gate_weight: float32 [2, 3072, 8448], P(None, 'ra', 'cb'), may hold values from -0.109375 to 0.109375
- gate_scale: float32 [2, 8448], P(None, 'cb'), may hold values from 0.5 to 2
- value_weight: float32 [2, 3072, 8448], P(None, 'ra', 'cb'), may hold values from -0.109375 to 0.109375
- value_scale: float32 [2, 8448], P(None, 'cb'), may hold values from 0.5 to 2
- gate_conv: float32 [2, 3, 8448], P(None, None, 'cb'), may hold values from -3.5 to 3.5
- value_conv: float32 [2, 3, 8448], P(None, None, 'cb'), may hold values from -3.5 to 3.5
- gate_bias: float32 [2, 8448], P(None, 'cb'), may hold values from -3 to 3
- value_bias: float32 [2, 8448], P(None, 'cb'), may hold values from -3 to 3
- down_weight: float32 [2, 8448, 3072], P(None, 'cb', 'ra'), may hold values from -0.0625 to 0.0625
- down_scale: float32 [2, 3072], P(None, 'ra'), may hold values from 0.5 to 2
Outputs:
- stream_out: bfloat16 [512, 3072], P(None, 'ra')
The draws below stay inside these ranges and needn't reach their ends.
Inputs may be any that keep to these rules, and one draw needn't show every extreme that they name: `tokens`: real values; within each token, the blocks of D // 16 consecutive features have scales that differ.
All inputs are finite; a program needn't handle non-finite values.
Results may differ from the reference program's by a relative error of at most 0.039.
Values may be sent and summed in bfloat16 or wider, within the bound.
A program may use at most 64 MiB of HBM per device.

```python
import math
import jax
import jax.numpy as jnp
from jax import lax

D = 3072
FF = 8448
TAPS = 3
LAYERS = 2
SEQ_LEN = 8
TOKENS = 512
N_CB = 8


def draw_tokens(key, part):
    first, second, third = jax.random.split(key, 3)
    scales = jnp.exp(jax.random.uniform(second, (TOKENS, 16), jnp.float32, -1.2, 1.2))
    widths = jnp.repeat(scales, D // 16, axis=1)
    base = jnp.clip(jax.random.normal(first, (TOKENS, D), jnp.float32), -4.0, 4.0)
    return (base * widths).astype(jnp.bfloat16)


def levels(own_key, dims, shards, smallest, top_value):
    loudness = 1.0
    for position, parts in shards:
        draws = jax.random.uniform(jax.random.fold_in(jax.random.fold_in(own_key, 6), position), (parts,), jnp.float32, smallest / len(shards), top_value / len(shards))
        loudness = loudness * jnp.repeat(jnp.exp(draws), dims[position] // parts).reshape((-1,) + (1,) * (len(dims) - 1 - position))
    return loudness


def centred(own_key, shape, scale, bound, cuts=(), kind=jnp.bfloat16):
    result = scale * jax.random.normal(own_key, shape, jnp.float32)
    if cuts:
        result = result * levels(own_key, shape, cuts, -0.22, 0.18)
    return jnp.clip(result, -bound, bound).astype(kind)


def setup_inputs(seed: int = 0) -> dict:
    arg_keys = jax.random.split(jax.random.key(seed), 13)
    tokens = draw_tokens(jax.random.fold_in(arg_keys[12], 71), 0)
    norm_gain = jnp.clip(1.0 + 0.18 * jax.random.normal(arg_keys[1], (LAYERS, D), jnp.float32), 0.1, 1.9)
    gate_weight = centred(arg_keys[2], (LAYERS, D, FF), D ** -0.5, 0.109375, ((1, 4), (2, 8)), jnp.float32)
    gate_scale = jnp.clip(jnp.exp(math.log(2.0) - 1.3862944 * jax.random.uniform(arg_keys[3], (LAYERS, FF), jnp.float32) ** levels(arg_keys[3], (LAYERS, FF), ((1, 8),), -0.2, 0.2)), 0.5, 2.0)
    value_weight = centred(arg_keys[4], (LAYERS, D, FF), D ** -0.5, 0.109375, ((1, 4), (2, 8)), jnp.float32)
    value_scale = jnp.clip(jnp.exp(math.log(2.0) - 1.3862944 * jax.random.uniform(arg_keys[5], (LAYERS, FF), jnp.float32) ** levels(arg_keys[5], (LAYERS, FF), ((1, 8),), -0.2, 0.2)), 0.5, 2.0)
    gate_conv = centred(arg_keys[6], (LAYERS, TAPS, FF), TAPS ** -0.5, 3.5, ((2, 8),), jnp.float32)
    value_conv = centred(arg_keys[7], (LAYERS, TAPS, FF), TAPS ** -0.5, 3.5, ((2, 8),), jnp.float32)
    gate_bias = centred(arg_keys[8], (LAYERS, FF), 0.5, 3.0, ((1, 8),), jnp.float32)
    value_bias = centred(arg_keys[9], (LAYERS, FF), 0.5, 3.0, ((1, 8),), jnp.float32)
    down_weight = centred(arg_keys[10], (LAYERS, FF, D), FF ** -0.5, 0.0625, ((1, 8), (2, 4)), jnp.float32)
    down_scale = jnp.clip(jnp.exp(math.log(2.0) - 1.3862944 * jax.random.uniform(arg_keys[11], (LAYERS, D), jnp.float32) ** levels(arg_keys[11], (LAYERS, D), ((1, 4),), -0.2, 0.2)), 0.5, 2.0)
    return {"tokens": tokens, "norm_gain": norm_gain, "gate_weight": gate_weight, "gate_scale": gate_scale, "value_weight": value_weight, "value_scale": value_scale, "gate_conv": gate_conv, "value_conv": value_conv, "gate_bias": gate_bias, "value_bias": value_bias, "down_weight": down_weight, "down_scale": down_scale}


epsilon = 1e-06
residual_keep = 0.5

def causal_conv(values, conv_taps, conv_bias):
    row_count, col_count = values.shape
    blocks = values.reshape(row_count // SEQ_LEN, SEQ_LEN, col_count)
    padded = jnp.pad(blocks, ((0, 0), (TAPS - 1, 0), (0, 0)))
    summed = conv_bias + jnp.zeros_like(blocks)
    for offset in range(TAPS):
        summed = summed + padded[:, offset:offset + SEQ_LEN] * conv_taps[offset]
    return summed.reshape(row_count, col_count)

def reference(tokens, norm_gain, gate_weight, gate_scale, value_weight, value_scale, gate_conv, value_conv, gate_bias, value_bias, down_weight, down_scale):
    stream = tokens
    for depth_index in range(LAYERS):
        widened = stream.astype(jnp.float32)
        squares = lax.optimization_barrier(jnp.sum(widened * widened, axis=1, keepdims=True))
        inverse_rms = lax.rsqrt(squares / D + epsilon)
        normed = (widened * norm_gain[depth_index]).astype(jnp.bfloat16)
        gate_pre = jnp.dot(normed, gate_weight[depth_index].astype(jnp.bfloat16), preferred_element_type=jnp.float32) * inverse_rms * gate_scale[depth_index]
        value_pre = jnp.dot(normed, value_weight[depth_index].astype(jnp.bfloat16), preferred_element_type=jnp.float32) * inverse_rms * value_scale[depth_index]
        gate_mixed = causal_conv(gate_pre, gate_conv[depth_index], gate_bias[depth_index])
        value_mixed = causal_conv(value_pre, value_conv[depth_index], value_bias[depth_index])
        hidden = (jax.nn.silu(gate_mixed) * value_mixed).astype(jnp.bfloat16)
        hidden = lax.optimization_barrier(hidden)
        pieces = hidden.astype(jnp.float32).reshape(TOKENS, N_CB, FF // N_CB)
        down_half = lax.optimization_barrier(down_weight[depth_index].astype(jnp.bfloat16))
        down_pieces = down_half.astype(jnp.float32).reshape(N_CB, FF // N_CB, D)
        partial_value = jnp.einsum('tcf,cfd->ctd', pieces, down_pieces)
        rounded = lax.optimization_barrier(partial_value.astype(jnp.bfloat16)).astype(jnp.float32)
        branch = lax.optimization_barrier(jnp.sum(rounded, axis=0)) * down_scale[depth_index]
        stream = (residual_keep * widened + branch).astype(jnp.bfloat16)
    return stream
```

```python
import functools
import jax
import jax.numpy as jnp
from jax import lax
from jax.experimental import pallas as pl
from jax.experimental.pallas import tpu as pltpu
from jax.sharding import PartitionSpec as P

SEQ_LEN = 8
EPSILON = 1e-06
RESIDUAL_KEEP = 0.5
MESH = pl.DeviceIdType.MESH
LANES = 128


def kernel(
    cfg,
    tokens_ref,
    gain_ref,
    gw_ref,
    gs_ref,
    vw_ref,
    vs_ref,
    gc_ref,
    vc_ref,
    gb_ref,
    vb_ref,
    dw_ref,
    ds_ref,
    out_ref,
    stage_g,
    stage_v,
    stage_d,
    wc,
    wd,
    par,
    xs,
    own,
    pin,
    pout,
    hid,
    ro,
    ri,
    w_sem,
    ps,
    pr,
    hs,
    hr,
    rs_s,
    rs_r,
    ag_s,
    ag_r,
):
    R, N, L, n, m, D, F = cfg
    Dl = tokens_ref.shape[1]
    rows = 2 * m
    own_rows = rows // N
    taps = gc_ref.shape[1]
    full = F // LANES * LANES
    rest = F - full
    wide = full + LANES
    sq_lane = 2 * rest
    S = max(n, 2 * R)
    z = lax.axis_index("ra")
    me = lax.axis_index("cb")

    def weight_copies(l):
        return (
            pltpu.make_async_copy(gw_ref.at[l], stage_g, w_sem.at[0]),
            pltpu.make_async_copy(vw_ref.at[l], stage_v, w_sem.at[1]),
            pltpu.make_async_copy(dw_ref.at[l], stage_d, w_sem.at[2]),
        )

    for copy in weight_copies(0):
        copy.start()

    barrier = pltpu.get_barrier_semaphore()
    for k in range(1, N):
        pl.semaphore_signal(
            barrier, inc=1, device_id={"cb": lax.rem(me + k, N)}, device_id_type=MESH
        )

    @pl.when(z > 0)
    def _():
        pl.semaphore_signal(barrier, inc=1, device_id={"ra": z - 1}, device_id_type=MESH)

    @pl.when(z < R - 1)
    def _():
        pl.semaphore_signal(barrier, inc=1, device_id={"ra": z + 1}, device_id_type=MESH)

    for i in range(n):
        block = tokens_ref[i * rows : (i + 1) * rows, :].astype(jnp.float32)
        xs[i] = block.reshape(N, own_rows, Dl).astype(jnp.bfloat16)

    par[...] = jnp.zeros_like(par)
    for l in range(L):
        par[l, 0:1, 0:F] = gs_ref[l : l + 1, :]
        par[l, 1:2, 0:F] = vs_ref[l : l + 1, :]
        par[l, 2:3, 0:F] = gb_ref[l : l + 1, :]
        par[l, 3:4, 0:F] = vb_ref[l : l + 1, :]
        par[l, 4 : 4 + taps, 0:F] = gc_ref[l]
        par[l, 4 + taps : 4 + 2 * taps, 0:F] = vc_ref[l]

    def cast_weights(l):
        copies = weight_copies(l)
        copies[0].wait()
        copies[1].wait()

        def up(b, carry):
            at = pl.ds(pl.multiple_of(b * 32, 32), 32)
            wc[l, at, 0:full] = stage_g[at, 0:full].astype(jnp.bfloat16)
            wc[l, at, full : 2 * full] = stage_v[at, 0:full].astype(jnp.bfloat16)
            tail = jnp.concatenate(
                [
                    stage_g[at, full:F],
                    stage_v[at, full:F],
                    jnp.zeros((32, LANES - 2 * rest), jnp.float32),
                ],
                axis=1,
            )
            wc[l, at, 2 * full : 2 * full + LANES] = tail.astype(jnp.bfloat16)
            return carry

        lax.fori_loop(0, Dl // 32, up, 0)
        copies[2].wait()

        def down(b, carry):
            at = pl.ds(pl.multiple_of(b * 32, 32), 32)
            wd[l, at, :] = stage_d[at, :].astype(jnp.bfloat16)
            return carry

        lax.fori_loop(0, F // 32, down, 0)
        wd[l, F:wide, :] = jnp.zeros((wide - F, Dl), jnp.bfloat16)

    cast_weights(0)
    for l in range(1, L):
        for copy in weight_copies(l):
            copy.start()

    expected = N - 1 + jnp.where(z > 0, 1, 0) + jnp.where(z < R - 1, 1, 0)
    pl.semaphore_wait(barrier, expected)

    def when_item(g, fn):
        layer = lax.div(g, S)
        i = lax.rem(g, S)

        @pl.when((g >= 0) & (g < L * S) & (i < n))
        def _():
            fn(layer, i, layer * n + i)

    def part_copy(q, d, target):
        return pltpu.make_async_remote_copy(
            src_ref=pout.at[q, d],
            dst_ref=pin.at[q, d],
            send_sem=ps.at[q, d],
            recv_sem=pr.at[q, d],
            device_id={"ra": target},
            device_id_type=MESH,
        )

    def hid_copy(q, d, target):
        return pltpu.make_async_remote_copy(
            src_ref=hid.at[q, d],
            dst_ref=hid.at[q, d],
            send_sem=hs.at[q, d],
            recv_sem=hr.at[q, d],
            device_id={"ra": target},
            device_id_type=MESH,
        )

    row_in_seq = lax.rem(lax.broadcasted_iota(jnp.int32, (m, wide), 0), SEQ_LEN)
    lane = lax.broadcasted_iota(jnp.int32, (m, LANES), 1)

    def conv(values, l, first):
        total = values * par[l, first + taps - 1 : first + taps, :]
        for back in range(1, taps):
            moved = jnp.where(row_in_seq >= back, pltpu.roll(values, back, 0), 0.0)
            total = total + moved * par[l, first + taps - 1 - back : first + taps - back, :]
        return total

    def finish(l, q, d, main_g, main_v, tail):
        squares = jnp.sum(
            jnp.where((lane == sq_lane) | (lane == sq_lane + 1), tail, 0.0),
            axis=1,
            keepdims=True,
        )
        inverse = lax.rsqrt(squares / D + EPSILON)
        gate = jnp.concatenate([main_g, tail], axis=1)
        value = jnp.concatenate([main_v, pltpu.roll(tail, LANES - rest, 1)], axis=1)
        gate = gate * inverse * par[l, 0:1, :]
        value = value * inverse * par[l, 1:2, :]
        gate = par[l, 2:3, :] + conv(gate, l, 4)
        value = par[l, 3:4, :] + conv(value, l, 4 + taps)
        hid[q, d] = (gate / (1.0 + jnp.exp(-gate)) * value).astype(jnp.bfloat16)

    def chain(d, l, q):
        first = (z == 0) if d == 0 else (z == R - 1)
        last = (z == R - 1) if d == 0 else (z == 0)
        ahead = z + 1 if d == 0 else z - 1
        behind = z - 1 if d == 0 else z + 1

        def send(main_g, main_v, tail):
            squares = jnp.sum(
                jnp.where((lane == sq_lane) | (lane == sq_lane + 1), tail, 0.0),
                axis=1,
                keepdims=True,
            )
            high = squares.astype(jnp.bfloat16).astype(jnp.float32)
            tail = jnp.where(
                lane == sq_lane,
                high,
                jnp.where(lane == sq_lane + 1, squares - high, tail),
            )
            pout[q, d, :, 0:full] = main_g.astype(jnp.bfloat16)
            pout[q, d, :, full : 2 * full] = main_v.astype(jnp.bfloat16)
            pout[q, d, :, 2 * full : 2 * full + LANES] = tail.astype(jnp.bfloat16)
            part_copy(q, d, ahead).start()

        def pieces(ref):
            return (
                ref[q, d, :, 0:full].astype(jnp.float32),
                ref[q, d, :, full : 2 * full].astype(jnp.float32),
                ref[q, d, :, 2 * full : 2 * full + LANES].astype(jnp.float32),
            )

        @pl.when(first)
        def _():
            send(*pieces(own))

        @pl.when(jnp.logical_not(first))
        def _():
            part_copy(q, d, behind).wait_recv()
            summed = tuple(a + b for a, b in zip(pieces(own), pieces(pin)))

            @pl.when(last)
            def _():
                finish(l, q, d, *summed)
                hid_copy(q, d, behind).start()

            @pl.when(jnp.logical_not(last))
            def _():
                send(*summed)

    def spread_back(d, l, q):
        source = z + 1 if d == 0 else z - 1
        onward = z - 1 if d == 0 else z + 1
        last = (z == 0) if d == 0 else (z == R - 1)
        hid_copy(q, d, source).wait_recv()

        @pl.when(jnp.logical_not(last))
        def _():
            hid_copy(q, d, onward).start()

    def peer_copy(src, dst, send_sem, recv_sem, peer):
        return pltpu.make_async_remote_copy(
            src_ref=src,
            dst_ref=dst,
            send_sem=send_sem,
            recv_sem=recv_sem,
            device_id={"cb": peer},
            device_id_type=MESH,
        )

    def wait_group(ref, q, sem):
        view = ref.at[q, 0 : N - 1]
        pltpu.make_async_copy(view, view, sem).wait()

    def down_and_scatter(l, i, q):
        h = hid[q].reshape(rows, wide)
        product = jnp.dot(h, wd[l], preferred_element_type=jnp.float32)
        ro[q] = product.reshape(N, own_rows, Dl).astype(jnp.bfloat16)
        for k in range(1, N):
            peer = lax.rem(me + k, N)
            peer_copy(
                ro.at[q, peer], ri.at[q, me], rs_s.at[q], rs_r.at[q], peer
            ).start()
        ri[q, me] = ro[q, me]

    def sum_and_gather(l, i, q):
        wait_group(ri, q, rs_r.at[q])
        total = ri[q, 0].astype(jnp.float32)
        for k in range(1, N):
            total = total + ri[q, k].astype(jnp.float32)
        branch = total * ds_ref[pl.ds(l, 1), :]
        fresh = RESIDUAL_KEEP * xs[q, me].astype(jnp.float32) + branch
        xs[q + n, me] = fresh.astype(jnp.bfloat16)
        for k in range(1, N):
            peer = lax.rem(me + k, N)
            peer_copy(
                xs.at[q + n, me], xs.at[q + n, me], ag_s.at[q], ag_r.at[q], peer
            ).start()

    def gathered(l, i, q):
        wait_group(xs, q + n, ag_r.at[q])

        @pl.when(l == L - 1)
        def _():
            block = xs[q + n].astype(jnp.float32).reshape(rows, Dl)
            at = pl.ds(pl.multiple_of(i * rows, rows), rows)
            out_ref[at, :] = block.astype(jnp.bfloat16)

    def products(l, i, q):
        x = xs[q].astype(jnp.float32).reshape(rows, Dl)
        squares = jnp.sum(x * x, axis=1, keepdims=True)
        normed = (x * gain_ref[pl.ds(l, 1), :]).astype(jnp.bfloat16)
        result = jnp.dot(normed, wc[l], preferred_element_type=jnp.float32)
        tail_lane = lax.broadcasted_iota(jnp.int32, (rows, LANES), 1)
        tail = jnp.where(tail_lane == sq_lane, squares, result[:, 2 * full :])
        for d in range(2):
            part = slice(d * m, (d + 1) * m)
            own[q, d, :, 0 : 2 * full] = result[part, 0 : 2 * full]
            own[q, d, :, 2 * full :] = tail[part]

    def slot(t, carry):
        when_item(t - 1 - z, lambda l, i, q: chain(0, l, q))
        when_item(t - R + z, lambda l, i, q: chain(1, l, q))

        @pl.when(z < R - 1)
        def _():
            when_item(t - 2 * R + 1 + z, lambda l, i, q: spread_back(0, l, q))

        @pl.when(z > 0)
        def _():
            when_item(t - R - z, lambda l, i, q: spread_back(1, l, q))

        when_item(t - 2 * R + 1, down_and_scatter)
        for l in range(1, L):

            @pl.when(t == l * S - 5)
            def _(l=l):
                cast_weights(l)

        when_item(t - 2 * R, gathered)
        when_item(t, products)
        when_item(t - 2 * R + 1, sum_and_gather)
        return carry

    lax.fori_loop(0, (L - 1) * S + n + 2 * R, slot, 0)

    def drain(q, carry):
        @pl.when(z < R - 1)
        def _():
            part_copy(q, 0, z + 1).wait_send()
            hid_copy(q, 1, z + 1).wait_send()

        @pl.when(z > 0)
        def _():
            part_copy(q, 1, z - 1).wait_send()
            hid_copy(q, 0, z - 1).wait_send()

        wait_group(ro, q, rs_s.at[q])
        wait_group(xs, q + n, ag_s.at[q])
        return carry

    lax.fori_loop(0, L * n, drain, 0)


def solution(mesh):
    R, N = mesh.shape["ra"], mesh.shape["cb"]

    def shards(*args):
        tokens, gw, gc = args[0], args[2], args[6]
        T, Dl = tokens.shape
        L, _, F = gw.shape
        m = 32
        rows = 2 * m
        n = T // rows
        full = F // LANES * LANES
        wide = full + LANES
        packed = 2 * full + LANES
        cfg = (R, N, L, n, m, Dl * R, F)
        Q = L * n
        bf16, f32 = jnp.bfloat16, jnp.float32
        dma = pltpu.SemaphoreType.DMA
        vmem = pl.BlockSpec(memory_space=pltpu.VMEM)
        hbm = pl.BlockSpec(memory_space=pl.ANY)
        in_specs = [hbm if k in (2, 4, 10) else vmem for k in range(12)]
        return pl.pallas_call(
            functools.partial(kernel, cfg),
            out_shape=jax.ShapeDtypeStruct((T, Dl), bf16),
            in_specs=in_specs,
            out_specs=vmem,
            scratch_shapes=[
                pltpu.VMEM((Dl, F), f32),
                pltpu.VMEM((Dl, F), f32),
                pltpu.VMEM((F, Dl), f32),
                pltpu.VMEM((L, Dl, packed), bf16),
                pltpu.VMEM((L, wide, Dl), bf16),
                pltpu.VMEM((L, 16, wide), f32),
                pltpu.VMEM((Q + n, N, rows // N, Dl), bf16),
                pltpu.VMEM((Q, 2, m, packed), f32),
                pltpu.VMEM((Q, 2, m, packed), bf16),
                pltpu.VMEM((Q, 2, m, packed), bf16),
                pltpu.VMEM((Q, 2, m, wide), bf16),
                pltpu.VMEM((Q, N, rows // N, Dl), bf16),
                pltpu.VMEM((Q, N, rows // N, Dl), bf16),
                dma((3,)),
                dma((Q, 2)),
                dma((Q, 2)),
                dma((Q, 2)),
                dma((Q, 2)),
                dma((Q,)),
                dma((Q,)),
                dma((Q,)),
                dma((Q,)),
            ],
            compiler_params=pltpu.CompilerParams(
                collective_id=0,
                has_side_effects=True,
                vmem_limit_bytes=67043328,
            ),
        )(*args)

    placed = (
        P(None, "ra"),
        P(None, "ra"),
        P(None, "ra", "cb"),
        P(None, "cb"),
        P(None, "ra", "cb"),
        P(None, "cb"),
        P(None, None, "cb"),
        P(None, None, "cb"),
        P(None, "cb"),
        P(None, "cb"),
        P(None, "cb", "ra"),
        P(None, "ra"),
    )
    return jax.shard_map(
        shards, mesh=mesh, in_specs=placed, out_specs=P(None, "ra"), check_vma=False
    )
```

```python
import functools
import jax
import jax.numpy as jnp
from jax import lax
from jax.experimental import pallas as pl
from jax.experimental.pallas import tpu as pltpu
from jax.sharding import PartitionSpec as P

SEQ_LEN = 8
EPSILON = 1e-06
RESIDUAL_KEEP = 0.5
MESH = pl.DeviceIdType.MESH
LANES = 128


def kernel(
    cfg,
    tokens_ref,
    gain_ref,
    gw_ref,
    gs_ref,
    vw_ref,
    vs_ref,
    gc_ref,
    vc_ref,
    gb_ref,
    vb_ref,
    dw_ref,
    ds_ref,
    out_ref,
    stage_g,
    stage_v,
    stage_d,
    wc,
    wd,
    par,
    xs,
    own,
    pin,
    pout,
    hid,
    ro,
    ri,
    w_sem,
    ps,
    pr,
    hs,
    hr,
    rs_s,
    rs_r,
    ag_s,
    ag_r,
):
    R, N, L, n, m, D, F = cfg
    Dl = tokens_ref.shape[1]
    rows = 2 * m
    own_rows = rows // N
    taps = gc_ref.shape[0]
    full = F // LANES * LANES
    rest = F - full
    wide = full + LANES
    sq_lane = 2 * rest
    S = max(n, 2 * R)
    z = lax.axis_index("ra")
    me = lax.axis_index("cb")

    def weight_copy(l, k):
        src, dst = ((gw_ref, stage_g), (vw_ref, stage_v), (dw_ref, stage_d))[k]
        return pltpu.make_async_copy(src.at[l], dst, w_sem.at[k])

    for k in range(3):
        weight_copy(0, k).start()

    barrier = pltpu.get_barrier_semaphore()
    for k in range(1, N):
        pl.semaphore_signal(
            barrier, inc=1, device_id={"cb": lax.rem(me + k, N)}, device_id_type=MESH
        )

    @pl.when(z > 0)
    def _():
        pl.semaphore_signal(barrier, inc=1, device_id={"ra": z - 1}, device_id_type=MESH)

    @pl.when(z < R - 1)
    def _():
        pl.semaphore_signal(barrier, inc=1, device_id={"ra": z + 1}, device_id_type=MESH)

    for i in range(n):
        block = tokens_ref[i * rows : (i + 1) * rows, :].astype(jnp.float32)
        xs[i] = block.reshape(N, own_rows, Dl).astype(jnp.bfloat16)

    par[...] = jnp.zeros_like(par)
    for l in range(L):
        par[l, 0:1, 0:F] = gs_ref[l : l + 1, :]
        par[l, 1:2, 0:F] = vs_ref[l : l + 1, :]
        par[l, 2:3, 0:F] = gb_ref[l : l + 1, :]
        par[l, 3:4, 0:F] = vb_ref[l : l + 1, :]
        for k in range(taps):
            par[l, 4 + k : 5 + k, 0:F] = gc_ref[k, l : l + 1, :]
            par[l, 4 + taps + k : 5 + taps + k, 0:F] = vc_ref[k, l : l + 1, :]

    def cast_rows(dst, l, first, src, start, count, step):
        def move(b, carry):
            to = pl.ds(pl.multiple_of(first + b * step, step), step)
            at = pl.ds(pl.multiple_of(start + b * step, step), step)
            dst[l, to, :] = src[at, :].astype(jnp.bfloat16)
            return carry

        lax.fori_loop(0, count // step, move, 0)

    def cast_up(l):
        weight_copy(l, 0).wait()
        cast_rows(wc, l, 0, stage_g, 0, full, 64)
        cast_rows(wc, l, 2 * full, stage_g, full, rest, 32)
        weight_copy(l, 1).wait()
        cast_rows(wc, l, full, stage_v, 0, full, 64)
        cast_rows(wc, l, 2 * full + rest, stage_v, full, rest, 32)
        wc[l, 2 * F :, :] = jnp.zeros((wc.shape[1] - 2 * F, Dl), jnp.bfloat16)
        if l + 1 < L:
            weight_copy(l + 1, 0).start()
            weight_copy(l + 1, 1).start()

    def cast_down(l):
        weight_copy(l, 2).wait()
        cast_rows(wd, l, 0, stage_d, 0, F, 32)
        wd[l, F:wide, :] = jnp.zeros((wide - F, Dl), jnp.bfloat16)
        if l + 1 < L:
            weight_copy(l + 1, 2).start()

    cast_up(0)

    expected = N - 1 + jnp.where(z > 0, 1, 0) + jnp.where(z < R - 1, 1, 0)
    pl.semaphore_wait(barrier, expected)

    def when_item(g, fn):
        layer = lax.div(g, S)
        i = lax.rem(g, S)

        @pl.when((g >= 0) & (g < L * S) & (i < n))
        def _():
            fn(layer, i, layer * n + i)

    def part_copy(q, d, target):
        return pltpu.make_async_remote_copy(
            src_ref=pout.at[q, d],
            dst_ref=pin.at[q, d],
            send_sem=ps.at[q, d],
            recv_sem=pr.at[q, d],
            device_id={"ra": target},
            device_id_type=MESH,
        )

    def hid_copy(q, d, target):
        return pltpu.make_async_remote_copy(
            src_ref=hid.at[q, d],
            dst_ref=hid.at[q, d],
            send_sem=hs.at[q, d],
            recv_sem=hr.at[q, d],
            device_id={"ra": target},
            device_id_type=MESH,
        )

    row_in_seq = lax.rem(lax.broadcasted_iota(jnp.int32, (m, wide), 0), SEQ_LEN)
    lane = lax.broadcasted_iota(jnp.int32, (m, LANES), 1)

    def conv(values, l, first):
        total = values * par[l, first + taps - 1 : first + taps, :]
        for back in range(1, taps):
            moved = jnp.where(row_in_seq >= back, pltpu.roll(values, back, 0), 0.0)
            total = total + moved * par[l, first + taps - 1 - back : first + taps - back, :]
        return total

    def finish(l, q, d, main_g, main_v, tail):
        squares = jnp.sum(
            jnp.where((lane == sq_lane) | (lane == sq_lane + 1), tail, 0.0),
            axis=1,
            keepdims=True,
        )
        inverse = lax.rsqrt(squares / D + EPSILON)
        gate = jnp.concatenate([main_g, tail], axis=1)
        value = jnp.concatenate([main_v, pltpu.roll(tail, LANES - rest, 1)], axis=1)
        gate = gate * inverse * par[l, 0:1, :]
        value = value * inverse * par[l, 1:2, :]
        gate = par[l, 2:3, :] + conv(gate, l, 4)
        value = par[l, 3:4, :] + conv(value, l, 4 + taps)
        hid[q, d] = (gate / (1.0 + jnp.exp(-gate)) * value).astype(jnp.bfloat16)

    def chain(d, l, q):
        first = (z == 0) if d == 0 else (z == R - 1)
        last = (z == R - 1) if d == 0 else (z == 0)
        ahead = z + 1 if d == 0 else z - 1
        behind = z - 1 if d == 0 else z + 1

        def send(main_g, main_v, tail):
            squares = jnp.sum(
                jnp.where((lane == sq_lane) | (lane == sq_lane + 1), tail, 0.0),
                axis=1,
                keepdims=True,
            )
            high = squares.astype(jnp.bfloat16).astype(jnp.float32)
            tail = jnp.where(
                lane == sq_lane,
                high,
                jnp.where(lane == sq_lane + 1, squares - high, tail),
            )
            pout[q, d, :, 0:full] = main_g.astype(jnp.bfloat16)
            pout[q, d, :, full : 2 * full] = main_v.astype(jnp.bfloat16)
            pout[q, d, :, 2 * full : 2 * full + LANES] = tail.astype(jnp.bfloat16)
            part_copy(q, d, ahead).start()

        def pieces(ref):
            return (
                ref[q, d, :, 0:full].astype(jnp.float32),
                ref[q, d, :, full : 2 * full].astype(jnp.float32),
                ref[q, d, :, 2 * full : 2 * full + LANES].astype(jnp.float32),
            )

        @pl.when(first)
        def _():
            send(*pieces(own))

        @pl.when(jnp.logical_not(first))
        def _():
            part_copy(q, d, behind).wait_recv()
            summed = tuple(a + b for a, b in zip(pieces(own), pieces(pin)))

            @pl.when(last)
            def _():
                finish(l, q, d, *summed)
                hid_copy(q, d, behind).start()

            @pl.when(jnp.logical_not(last))
            def _():
                send(*summed)

    def spread_back(d, l, q):
        source = z + 1 if d == 0 else z - 1
        onward = z - 1 if d == 0 else z + 1
        last = (z == 0) if d == 0 else (z == R - 1)
        hid_copy(q, d, source).wait_recv()

        @pl.when(jnp.logical_not(last))
        def _():
            hid_copy(q, d, onward).start()

    def peer_copy(src, dst, send_sem, recv_sem, peer):
        return pltpu.make_async_remote_copy(
            src_ref=src,
            dst_ref=dst,
            send_sem=send_sem,
            recv_sem=recv_sem,
            device_id={"cb": peer},
            device_id_type=MESH,
        )

    def wait_group(ref, q, sem):
        view = ref.at[q, 0 : N - 1]
        pltpu.make_async_copy(view, view, sem).wait()

    def down_and_scatter(l, i, q):
        h = hid[q].reshape(rows, wide)
        product = jnp.dot(h, wd[l], preferred_element_type=jnp.float32)
        ro[q] = product.reshape(N, own_rows, Dl).astype(jnp.bfloat16)
        for k in range(1, N):
            peer = lax.rem(me + k, N)
            peer_copy(
                ro.at[q, peer], ri.at[q, me], rs_s.at[q], rs_r.at[q], peer
            ).start()
        ri[q, me] = ro[q, me]

    def sum_and_gather(l, i, q):
        wait_group(ri, q, rs_r.at[q])
        total = ri[q, 0].astype(jnp.float32)
        for k in range(1, N):
            total = total + ri[q, k].astype(jnp.float32)
        branch = total * ds_ref[pl.ds(l, 1), :]
        fresh = RESIDUAL_KEEP * xs[q, me].astype(jnp.float32) + branch
        xs[q + n, me] = fresh.astype(jnp.bfloat16)
        for k in range(1, N):
            peer = lax.rem(me + k, N)
            peer_copy(
                xs.at[q + n, me], xs.at[q + n, me], ag_s.at[q], ag_r.at[q], peer
            ).start()

    def gathered(l, i, q):
        wait_group(xs, q + n, ag_r.at[q])

        @pl.when(l == L - 1)
        def _():
            block = xs[q + n].astype(jnp.float32).reshape(rows, Dl)
            at = pl.ds(pl.multiple_of(i * rows, rows), rows)
            out_ref[at, :] = block.astype(jnp.bfloat16)

    def products(l, i, q):
        x = xs[q].astype(jnp.float32).reshape(rows, Dl)
        squares = jnp.sum(x * x, axis=1, keepdims=True)
        normed = (x * gain_ref[pl.ds(l, 1), :]).astype(jnp.bfloat16)
        result = lax.dot_general(
            normed,
            wc[l],
            (((1,), (1,)), ((), ())),
            preferred_element_type=jnp.float32,
        )
        tail_lane = lax.broadcasted_iota(jnp.int32, (rows, LANES), 1)
        tail = jnp.where(tail_lane == sq_lane, squares, result[:, 2 * full :])
        for d in range(2):
            part = slice(d * m, (d + 1) * m)
            own[q, d, :, 0 : 2 * full] = result[part, 0 : 2 * full]
            own[q, d, :, 2 * full :] = tail[part]

    def slot(t, carry):
        when_item(t - 1 - z, lambda l, i, q: chain(0, l, q))
        when_item(t - R + z, lambda l, i, q: chain(1, l, q))

        @pl.when(z < R - 1)
        def _():
            when_item(t - 2 * R + 1 + z, lambda l, i, q: spread_back(0, l, q))

        @pl.when(z > 0)
        def _():
            when_item(t - R - z, lambda l, i, q: spread_back(1, l, q))

        when_item(t - 2 * R + 1, down_and_scatter)
        for l in range(L):
            if l:
                pl.when(t == l * S - 4)(functools.partial(cast_up, l))
            pl.when(t == l * S + 1)(functools.partial(cast_down, l))

        when_item(t - 2 * R, gathered)
        when_item(t, products)
        when_item(t - 2 * R + 1, sum_and_gather)
        return carry

    lax.fori_loop(0, (L - 1) * S + n + 2 * R, slot, 0)

    def drain(q, carry):
        @pl.when(z < R - 1)
        def _():
            part_copy(q, 0, z + 1).wait_send()
            hid_copy(q, 1, z + 1).wait_send()

        @pl.when(z > 0)
        def _():
            part_copy(q, 1, z - 1).wait_send()
            hid_copy(q, 0, z - 1).wait_send()

        wait_group(ro, q, rs_s.at[q])
        wait_group(xs, q + n, ag_s.at[q])
        return carry

    lax.fori_loop(0, L * n, drain, 0)


def solution(mesh):
    R, N = mesh.shape["ra"], mesh.shape["cb"]

    def shards(*args):
        args = list(args)
        for k in (2, 4):
            args[k] = jnp.swapaxes(args[k], 1, 2)
        for k in (6, 7):
            args[k] = jnp.swapaxes(args[k], 0, 1)
        tokens, gw = args[0], args[2]
        T, Dl = tokens.shape
        L, F, _ = gw.shape
        m = 32
        rows = 2 * m
        n = T // rows
        full = F // LANES * LANES
        wide = full + LANES
        packed = 2 * full + LANES
        cfg = (R, N, L, n, m, Dl * R, F)
        Q = L * n
        bf16, f32 = jnp.bfloat16, jnp.float32
        dma = pltpu.SemaphoreType.DMA
        vmem = pl.BlockSpec(memory_space=pltpu.VMEM)
        hbm = pl.BlockSpec(memory_space=pl.ANY)
        in_specs = [hbm if k in (2, 4, 10) else vmem for k in range(12)]
        return pl.pallas_call(
            functools.partial(kernel, cfg),
            out_shape=jax.ShapeDtypeStruct((T, Dl), bf16),
            in_specs=in_specs,
            out_specs=vmem,
            scratch_shapes=[
                pltpu.VMEM((F, Dl), f32),
                pltpu.VMEM((F, Dl), f32),
                pltpu.VMEM((F, Dl), f32),
                pltpu.VMEM((L, packed, Dl), bf16),
                pltpu.VMEM((L, wide, Dl), bf16),
                pltpu.VMEM((L, 16, wide), f32),
                pltpu.VMEM((Q + n, N, rows // N, Dl), bf16),
                pltpu.VMEM((Q, 2, m, packed), f32),
                pltpu.VMEM((Q, 2, m, packed), bf16),
                pltpu.VMEM((Q, 2, m, packed), bf16),
                pltpu.VMEM((Q, 2, m, wide), bf16),
                pltpu.VMEM((Q, N, rows // N, Dl), bf16),
                pltpu.VMEM((Q, N, rows // N, Dl), bf16),
                dma((3,)),
                dma((Q, 2)),
                dma((Q, 2)),
                dma((Q, 2)),
                dma((Q, 2)),
                dma((Q,)),
                dma((Q,)),
                dma((Q,)),
                dma((Q,)),
            ],
            compiler_params=pltpu.CompilerParams(
                collective_id=0,
                has_side_effects=True,
                vmem_limit_bytes=67043328,
            ),
        )(*args)

    placed = (
        P(None, "ra"),
        P(None, "ra"),
        P(None, "ra", "cb"),
        P(None, "cb"),
        P(None, "ra", "cb"),
        P(None, "cb"),
        P(None, None, "cb"),
        P(None, None, "cb"),
        P(None, "cb"),
        P(None, "cb"),
        P(None, "cb", "ra"),
        P(None, "ra"),
    )
    return jax.shard_map(
        shards, mesh=mesh, in_specs=placed, out_specs=P(None, "ra"), check_vma=False
    )
```
